512 devices in a mesh: ep: 16 (over y, x), tp: 32 (over z, core).
Axes of the slice: x: 4, y: 4, z: 16, core: 2. Of those that a mesh axis runs over, the one named last changes fastest.
Arguments:
- tokens: bfloat16 [4096, 2048], P('ep', 'tp'), may hold values from -600 to 600
- pre_gain: float32 [2048], P('tp'), may hold values from 0.1 to 1.9
- expert_gate: bfloat16 [16, 2048, 8192], P('ep', None, 'tp'), may hold values from -0.125 to 0.125
- expert_up: bfloat16 [16, 2048, 8192], P('ep', None, 'tp'), may hold values from -0.125 to 0.125
- expert_down: bfloat16 [16, 8192, 2048], P('ep', 'tp'), may hold values from -8 to 8
- routes: int32 [4096, 2], P('ep'), may hold values from 0 to 15, all different within a row; in each aligned block of 256 rows (0 to 255, 256 to 511, ...) at most 48 rows name the same one
- route_weights: float32 [4096, 2], P('ep'), may hold values from 0.1 to 1
- post_gain: float32 [2048], P('tp'), may hold values from 0.1 to 1.9
Outputs:
- layer_out: bfloat16 [4096, 2048], P('ep', 'tp')
The draws below stay inside these ranges and needn't reach their ends.
Inputs may be any that keep to these rules, and one draw needn't show every extreme that they name: `routes`: each token names 2 different experts. Among the 256 tokens of one index of ep no expert is named more than 48 times, a bound that some expert reaches in some of these blocks.
All inputs are finite; a program needn't handle non-finite values.
Results may differ from the reference program's by a relative error of at most 0.024.
Values may be sent and summed in bfloat16 or wider, within the bound.
No kernel may reach another device: no remote copies, remote signals or barrier semaphores. Data moves between devices by JAX's collectives and lax.ppermute only.
A program may use at most 64 MiB of HBM per device.

```python
import math
import jax
import jax.numpy as jnp
import numpy as np
from jax import lax

D = 2048
FF = 8192
TOPK = 2
TOK_EP = 256
EXPERTS = 16
CAP = 48
TOKENS = 4096
N_EP = 16
N_TP = 32


def column_scale(key, count):
    ramp = jnp.arange(count, dtype=jnp.float32) / max(count - 1, 1)
    rough = jax.random.uniform(key, (count,), jnp.float32, -0.35, 0.35)
    return jnp.exp(math.log(10.0) * ramp + rough)


def draw_tokens(key, part):
    keys = jax.random.split(jax.random.fold_in(key, 11), 3)
    entries = jnp.clip(jax.random.normal(keys[0], (TOKENS, D), jnp.float32), -4.0, 4.0)
    row_scale = jnp.exp(jax.random.uniform(keys[1], (TOKENS, 1), jnp.float32, 0.0, math.log(10.0)))
    return (entries * row_scale * column_scale(keys[2], D)[None, :]).astype(jnp.bfloat16)


def draw_expert_down(key, part):
    keys = jax.random.split(jax.random.fold_in(key, 23), 2)
    entries = jnp.clip(jax.random.normal(keys[0], (EXPERTS, FF, D), jnp.float32), -4.0, 4.0)
    scaled = entries * FF ** (-0.5) * column_scale(keys[1], D)[None, None, :]
    return scaled.astype(jnp.bfloat16)


def shard_levels(stream_key, extent, cuts, least, top_value):
    level = 1.0
    for axis_at, shards_of in cuts:
        heights = jax.random.uniform(jax.random.fold_in(jax.random.fold_in(stream_key, 6), axis_at), (shards_of,), jnp.float32, least / len(cuts), top_value / len(cuts))
        level = level * jnp.repeat(jnp.exp(heights), extent[axis_at] // shards_of).reshape((-1,) + (1,) * (len(extent) - 1 - axis_at))
    return level


def shared_out(key, own, number, rows, amount, top, limit, skew):
    ranking = jax.random.permutation(key, amount)
    crowded, usual = shares(amount, rows * top, limit, skew, True), shares(amount, rows * top, limit, skew, False)
    places = jnp.arange(amount)

    def named(lengths, offset_by):
        used = int((lengths > 0).sum())
        fixed = max(1, used // 4)
        shifted = fixed + (places - fixed + offset_by * (used - fixed)) % max(1, amount - fixed)
        return jnp.zeros((amount,), jnp.int32).at[ranking[jnp.where(places < fixed, places, shifted)]].set(jnp.asarray(lengths, jnp.int32))

    lengths = jnp.where(number % 4 == 0, named(crowded, number // 4), named(usual, number - number // 4 - 1))
    mixed = jax.random.permutation(jax.random.fold_in(own, 3), amount)
    source_of, receiver = mixed[0:amount // 2 * 2:2], mixed[1:amount // 2 * 2:2]
    margin = jnp.minimum(lengths[source_of] - 1, limit - lengths[receiver]) // 2
    margin = jnp.where((source_of == ranking[0]) | (receiver == ranking[0]) | (lengths[receiver] == 0), 0, jnp.maximum(margin, 0))
    shifted = jax.random.randint(jax.random.fold_in(own, 4), (amount // 2,), 0, 1 << 20) % (margin + 1)
    lengths = lengths.at[source_of].add(-shifted).at[receiver].add(shifted)
    items = jnp.searchsorted(jnp.cumsum(lengths), jnp.arange(rows * top), side="right").astype(jnp.int32)
    table = items.reshape(top, rows).T
    table = table[jax.random.permutation(jax.random.fold_in(own, 1), rows)]
    offset_by = jax.random.randint(jax.random.fold_in(own, 2), (rows, 1), 0, top)
    return jnp.take_along_axis(table, (jnp.arange(top)[None, :] + offset_by) % top, axis=1)


def shares(amount, total, reach, slope, full):
    weights = [(1 << 20) // math.isqrt(grade ** slope) + 1 for grade in range(1, amount + 1)]
    largest = reach if full else min(reach, max(-(-total // amount), total * weights[0] // sum(weights)))
    least = 1 if total - largest >= amount - 1 else 0
    counts, rest = [largest] + [least] * (amount - 1), total - largest - least * (amount - 1)
    while rest > 0:
        candidates = [i for i in range(1, amount) if counts[i] < largest] or [i for i in range(1, amount) if counts[i] < reach]
        mass, left = sum([weights[i] for i in candidates]), rest
        for i in candidates:
            extra = min(reach - counts[i], max(1, left * weights[i] // mass), rest)
            counts[i] = counts[i] + extra
            rest = rest - extra
    return np.array(counts)


def gaussian(stream_key, dims, spread, most, cuts=(), held_as=jnp.bfloat16):
    values = spread * jax.random.normal(stream_key, dims, jnp.float32)
    if cuts:
        values = values * shard_levels(stream_key, dims, cuts, -0.22, 0.18)
    return jnp.clip(values, -most, most).astype(held_as)


def setup_inputs(seed: int = 0) -> dict:
    key_of = jax.random.split(jax.random.key(seed), 9)
    tokens = draw_tokens(jax.random.fold_in(key_of[8], 71), 0)
    pre_gain = jnp.clip(1.0 + 0.18 * jax.random.normal(key_of[1], (D,), jnp.float32), 0.1, 1.9)
    expert_gate = gaussian(key_of[2], (EXPERTS, D, FF), D ** -0.5, 0.125, ((0, 16), (2, 32)))
    expert_up = gaussian(key_of[3], (EXPERTS, D, FF), D ** -0.5, 0.125, ((0, 16), (2, 32)))
    expert_down = draw_expert_down(jax.random.fold_in(key_of[8], 71), 0)
    routes_keys = jax.random.split(jax.random.fold_in(key_of[5], 1), TOKENS // TOK_EP)
    routes_turns = jax.random.permutation(jax.random.fold_in(key_of[5], 3), TOKENS // TOK_EP)
    routes = jax.vmap(lambda own, number: shared_out(jax.random.fold_in(key_of[5], 2), own, number, TOK_EP, EXPERTS, TOPK, CAP, 2))(routes_keys, routes_turns).reshape((TOKENS, TOPK))
    route_weights = jnp.clip(0.1 + 0.9 * jax.random.uniform(key_of[6], (TOKENS, TOPK), jnp.float32) ** shard_levels(key_of[6], (TOKENS, TOPK), ((0, 16),), -0.2, 0.2), 0.1, 1.0)
    post_gain = jnp.clip(1.0 + 0.18 * jax.random.normal(key_of[7], (D,), jnp.float32), 0.1, 1.9)
    return {"tokens": tokens, "pre_gain": pre_gain, "expert_gate": expert_gate, "expert_up": expert_up, "expert_down": expert_down, "routes": routes, "route_weights": route_weights, "post_gain": post_gain}


EPSILON = 1e-06

def rms_scale(values, gain):
    return values * lax.rsqrt(lax.optimization_barrier(jnp.mean(values * values, axis=-1, keepdims=True)) + EPSILON) * gain.astype(jnp.float32)

def reference(tokens, pre_gain, expert_gate, expert_up, expert_down, routes, route_weights, post_gain):
    normed = rms_scale(tokens.astype(jnp.float32), pre_gain).astype(jnp.bfloat16)
    blocks = routes.reshape(N_EP, TOK_EP, TOPK).astype(jnp.int32)
    onehot = (blocks[..., None] == jnp.arange(EXPERTS, dtype=jnp.int32)).astype(jnp.int32)
    onehot = onehot.reshape(N_EP, TOK_EP * TOPK, EXPERTS)
    earlier = jnp.cumsum(onehot, axis=1) - onehot
    slots = lax.optimization_barrier(jnp.sum(earlier * onehot, axis=-1)).reshape(N_EP, TOK_EP, TOPK).astype(jnp.int32)
    block_ids = jnp.broadcast_to(jnp.arange(N_EP, dtype=jnp.int32)[:, None, None], blocks.shape)
    token_ids = jnp.broadcast_to(block_ids * TOK_EP + jnp.arange(TOK_EP, dtype=jnp.int32)[None, :, None], blocks.shape)
    table = jnp.full((EXPERTS, N_EP, CAP), TOKENS, jnp.int32).at[blocks, block_ids, slots].set(token_ids)
    padded = jnp.concatenate([normed, jnp.zeros((1, D), jnp.bfloat16)], axis=0)
    row_count = N_EP * CAP
    part_units = FF // N_TP

    def one_expert(args):
        row_index, w_gate, w_up, w_down = args
        rows = padded[row_index.reshape(-1)]
        gate_pre = jnp.dot(rows, w_gate, preferred_element_type=jnp.float32)
        up_pre = jnp.dot(rows, w_up, preferred_element_type=jnp.float32)
        hidden = (jax.nn.silu(gate_pre) * up_pre).astype(jnp.bfloat16)
        hidden_blocks = hidden.reshape(row_count, N_TP, part_units).transpose(1, 0, 2)
        weight_blocks = w_down.reshape(N_TP, part_units, D)

        def add_block(running, pair):
            part_hidden, part_weight = pair
            partial_value = jnp.dot(part_hidden, part_weight, preferred_element_type=jnp.float32)
            rounded = lax.optimization_barrier(partial_value.astype(jnp.bfloat16))
            return (running + rounded.astype(jnp.float32), None)
        running, _ = lax.scan(add_block, jnp.zeros((row_count, D), jnp.float32), (hidden_blocks, weight_blocks))
        return running.astype(jnp.bfloat16)
    outputs = lax.map(one_expert, (table, expert_gate, expert_up, expert_down))
    picked = outputs[blocks, block_ids * CAP + slots].reshape(TOKENS, TOPK, D)
    combined = lax.optimization_barrier(jnp.sum(route_weights[:, :, None] * picked.astype(jnp.float32), axis=1))
    return rms_scale(combined, post_gain).astype(jnp.bfloat16)
```

```python
import jax
import jax.numpy as jnp
from jax import lax
from jax.experimental import pallas as pl
from jax.experimental.pallas import tpu as pltpu
from jax.sharding import Mesh
from jax.sharding import PartitionSpec as P

TP = ("tp_0", "tp_1")
EPSILON = 1e-06
F32 = jnp.float32
BF16 = jnp.bfloat16


def sent_to_all(value, axis):
    copies = jnp.broadcast_to(value, (lax.axis_size(axis), *value.shape))
    return lax.all_to_all(copies, axis, split_axis=0, concat_axis=0, tiled=True)


def swapped(value):
    return lax.ppermute(value, "tp_1", [(0, 1), (1, 0)])


def three_pieces(value):
    high = lax.reduce_precision(value, 8, 7)
    middle = lax.reduce_precision(value - high, 8, 7)
    low = lax.reduce_precision(value - high - middle, 8, 7)
    return jnp.stack([high, middle, low]).astype(BF16)


def expert_kernel(core, own, peer, gate, up, down, keep, send, split_down):
    mine = core[0]
    other = 1 - mine
    half = own.shape[1]
    hidden_units = gate.shape[-1]
    row = lax.broadcasted_iota(jnp.int32, (256, 256), 0)
    col = lax.broadcasted_iota(jnp.int32, (256, 256), 1)
    source = ((col // 64) % 2) * 128 + (col // 128) * 64 + col % 64
    shuffle = (row == source).astype(F32).astype(BF16)
    for block in range(down.shape[1] // 256):
        turned = jnp.dot(
            down[:, block * 256 : block * 256 + 256], shuffle, preferred_element_type=F32
        ).astype(BF16)
        for side in range(2):
            split_down[side, :, block * 128 : block * 128 + 128] = turned[
                :, side * 128 : side * 128 + 128
            ]
    gate_own = gate[:, mine].reshape(half, hidden_units)
    gate_peer = gate[:, other].reshape(half, hidden_units)
    up_own = up[:, mine].reshape(half, hidden_units)
    up_peer = up[:, other].reshape(half, hidden_units)
    down_own = split_down[mine]
    down_peer = split_down[other]
    step = 256
    for start in range(0, own.shape[0], step):
        here = slice(start, start + step)
        a, b = own[here, :], peer[here, :]
        gate_pre = jnp.dot(a, gate_own, preferred_element_type=F32) + jnp.dot(
            b, gate_peer, preferred_element_type=F32
        )
        up_pre = jnp.dot(a, up_own, preferred_element_type=F32) + jnp.dot(
            b, up_peer, preferred_element_type=F32
        )
        hidden = (gate_pre / (1.0 + jnp.exp(-gate_pre)) * up_pre).astype(BF16)
        send[here, :] = jnp.dot(hidden, down_peer, preferred_element_type=F32).astype(BF16)
        keep[here, :] = jnp.dot(hidden, down_own, preferred_element_type=F32).astype(BF16)


def local(tokens, pre_gain, expert_gate, expert_up, expert_down, routes, route_weights, post_gain):
    groups = lax.axis_size("ep")
    columns = lax.axis_size("tp_0")
    tok_rows, part_width = tokens.shape
    full_width = part_width * lax.axis_size(TP)
    half_width = part_width * columns
    capacity = 3 * tok_rows // groups
    slots_all = groups * capacity
    core = lax.axis_index("tp_1").astype(jnp.int32)

    values = tokens.T.astype(F32)
    partial_sq = jnp.sum(values * values, axis=0)
    scaled = (values * pre_gain[:, None]).astype(BF16)
    pieces = jnp.pad(three_pieces(partial_sq), ((0, 5), (0, 0)))
    payload = jnp.concatenate([scaled, pieces], axis=0)
    gathered = lax.all_gather(payload, "tp_0", axis=0, tiled=False)
    half_sq = jnp.sum(gathered[:, part_width : part_width + 3].astype(F32), axis=(0, 1))
    input_sq = half_sq + swapped(half_sq[None])[0]
    row_scale = lax.rsqrt(input_sq / full_width + EPSILON)
    normed = (
        (gathered[:, :part_width].astype(F32) * row_scale).astype(BF16).reshape(half_width, tok_rows)
    )

    chosen = routes.T
    experts = lax.broadcasted_iota(jnp.int32, (groups, tok_rows), 0)
    first_hot = (experts == chosen[0]).astype(F32)
    second_hot = (experts == chosen[1]).astype(F32)
    before = (
        lax.broadcasted_iota(jnp.int32, (tok_rows, tok_rows), 0)
        < lax.broadcasted_iota(jnp.int32, (tok_rows, tok_rows), 1)
    ).astype(BF16)
    earlier = jnp.dot(
        (first_hot + second_hot).astype(BF16), before, preferred_element_type=F32
    )
    first_slot = jnp.sum(earlier * first_hot, axis=0).astype(jnp.int32)
    second_slot = jnp.sum(earlier * second_hot, axis=0).astype(jnp.int32)
    places = lax.broadcasted_iota(jnp.int32, (slots_all, tok_rows), 0)
    first_pick = (places == chosen[0] * capacity + first_slot).astype(BF16)
    second_pick = (places == chosen[1] * capacity + second_slot).astype(BF16)

    outgoing = lax.dot_general(
        first_pick + second_pick, normed, (((1,), (1,)), ((), ())), preferred_element_type=F32
    ).astype(BF16)
    own = lax.all_to_all(
        outgoing.reshape(groups, capacity, half_width), "ep", split_axis=0, concat_axis=0, tiled=True
    ).reshape(slots_all, half_width)
    peer = swapped(own)

    vmem = pl.BlockSpec(memory_space=pltpu.VMEM)
    units = expert_gate.shape[-1]
    keep, send = pl.pallas_call(
        expert_kernel,
        in_specs=[pl.BlockSpec(memory_space=pltpu.SMEM), vmem, vmem, vmem, vmem, vmem],
        out_specs=[vmem, vmem],
        out_shape=[jax.ShapeDtypeStruct((slots_all, half_width), BF16)] * 2,
        scratch_shapes=[pltpu.VMEM((2, units, half_width), BF16)],
        compiler_params=pltpu.CompilerParams(vmem_limit_bytes=48 * 1024 * 1024),
        name="expert",
    )(
        core[None],
        own,
        peer,
        expert_gate.reshape(columns, 2, part_width, units),
        expert_up.reshape(columns, 2, part_width, units),
        expert_down.reshape(units, full_width),
    )
    expert_out = (keep.astype(F32) + swapped(send).astype(F32)).astype(BF16)
    returned = lax.all_to_all(
        expert_out.reshape(groups, capacity, half_width), "ep", split_axis=0, concat_axis=0, tiled=True
    ).reshape(slots_all, half_width)

    contract = (((0,), (0,)), ((), ()))
    first_out = lax.dot_general(returned, first_pick, contract, preferred_element_type=F32)
    second_out = lax.dot_general(returned, second_pick, contract, preferred_element_type=F32)
    weights = route_weights.T
    partial = (weights[0] * first_out + weights[1] * second_out).astype(BF16)
    parts = lax.all_to_all(
        partial.reshape(columns, part_width, tok_rows), "tp_0", split_axis=0, concat_axis=0, tiled=True
    )
    combined = jnp.sum(parts.astype(F32), axis=0)
    output_sq = jnp.sum(sent_to_all(jnp.sum(combined * combined, axis=0)[None], TP), axis=(0, 1))
    result = combined * lax.rsqrt(output_sq / full_width + EPSILON) * post_gain[:, None]
    return result.astype(BF16).T


def solution(mesh):
    torus = Mesh(mesh.devices.reshape(mesh.shape["ep"], 16, 2), ("ep", "tp_0", "tp_1"))
    in_specs = (
        P("ep", TP),
        P(TP),
        P("ep", None, TP),
        P("ep", None, TP),
        P("ep", TP, None),
        P("ep", None),
        P("ep", None),
        P(TP),
    )
    out_specs = P("ep", TP)
    return jax.shard_map(local, mesh=torus, in_specs=in_specs, out_specs=out_specs, check_vma=False)
```

```python
import jax
import jax.numpy as jnp
from jax import lax
from jax.experimental import pallas as pl
from jax.experimental.pallas import tpu as pltpu
from jax.sharding import Mesh
from jax.sharding import PartitionSpec as P

Z = ("z8", "zp")
TP = ("z8", "zp", "tp_1")
EPSILON = 1e-06
F32 = jnp.float32
BF16 = jnp.bfloat16
STEP = 384
MIB = 1024 * 1024


def sent_to_all(value, axis):
    copies = jnp.broadcast_to(value, (lax.axis_size(axis), *value.shape))
    return lax.all_to_all(copies, axis, split_axis=0, concat_axis=0, tiled=True)


def swapped(value):
    return lax.ppermute(value, "tp_1", [(0, 1), (1, 0)])


def three_pieces(value):
    high = lax.reduce_precision(value, 8, 7)
    middle = lax.reduce_precision(value - high, 8, 7)
    low = lax.reduce_precision(value - high - middle, 8, 7)
    return jnp.stack([high, middle, low]).astype(BF16)


def own_half_kernel(core, own, gate, up, down, gate_pre, up_pre, split_down):
    mine = core[0]
    half = own.shape[1]
    hidden_units = gate.shape[-1]
    gate_own = gate[:, mine].reshape(half, hidden_units)
    up_own = up[:, mine].reshape(half, hidden_units)
    for start in range(0, own.shape[0], STEP):
        here = slice(start, start + STEP)
        rows = own[here, :]
        gate_pre[here, :] = jnp.dot(rows, gate_own, preferred_element_type=F32)
        up_pre[here, :] = jnp.dot(rows, up_own, preferred_element_type=F32)
    size = 512
    row = lax.broadcasted_iota(jnp.int32, (size, size), 0)
    col = lax.broadcasted_iota(jnp.int32, (size, size), 1)
    part = col // 64
    source = (part % 2) * 256 + ((part // 2) % 2) * 128 + (part // 4) * 64 + col % 64
    shuffle = (row == source).astype(F32).astype(BF16)
    for block in range(down.shape[1] // size):
        turned = jnp.dot(
            down[:, block * size : (block + 1) * size], shuffle, preferred_element_type=F32
        ).astype(BF16)
        for side in range(2):
            for pair in range(2):
                split_down[side, pair, :, block * 128 : block * 128 + 128] = turned[
                    :, side * 256 + pair * 128 : side * 256 + pair * 128 + 128
                ]


def peer_half_kernel(core, peer, gate_own, up_own, gate, up, split_down, hidden, send):
    other = 1 - core[0]
    half = peer.shape[1]
    hidden_units = gate.shape[-1]
    gate_peer = gate[:, other].reshape(half, hidden_units)
    up_peer = up[:, other].reshape(half, hidden_units)
    capacity = send.shape[2]
    for start in range(0, peer.shape[0], STEP):
        here = slice(start, start + STEP)
        there = slice(start // capacity, (start + STEP) // capacity)
        rows = peer[here, :]
        gate_pre = gate_own[here, :] + jnp.dot(rows, gate_peer, preferred_element_type=F32)
        up_pre = up_own[here, :] + jnp.dot(rows, up_peer, preferred_element_type=F32)
        value = (gate_pre / (1.0 + jnp.exp(-gate_pre)) * up_pre).astype(BF16)
        hidden[here, :] = value
        for pair in range(2):
            part = jnp.dot(value, split_down[other, pair], preferred_element_type=F32)
            send[there, pair] = part.astype(BF16).reshape(STEP // capacity, capacity, -1)


def keep_kernel(core, hidden, split_down, keep):
    mine = core[0]
    capacity = keep.shape[2]
    for start in range(0, hidden.shape[0], STEP):
        there = slice(start // capacity, (start + STEP) // capacity)
        value = hidden[start : start + STEP, :]
        for pair in range(2):
            part = jnp.dot(value, split_down[mine, pair], preferred_element_type=F32)
            keep[there, pair] = part.astype(BF16).reshape(STEP // capacity, capacity, -1)


def local(tokens, pre_gain, expert_gate, expert_up, expert_down, routes, route_weights, post_gain):
    groups = lax.axis_size("ep")
    columns = lax.axis_size(Z)
    pairs = lax.axis_size("zp")
    tok_rows, part_width = tokens.shape
    full_width = part_width * lax.axis_size(TP)
    half_width = part_width * columns
    capacity = 3 * tok_rows // groups
    slots_all = groups * capacity
    core = lax.axis_index("tp_1").astype(jnp.int32)

    values = tokens.T.astype(F32)
    partial_sq = jnp.sum(values * values, axis=0)
    scaled = (values * pre_gain[:, None]).astype(BF16)
    pieces = jnp.pad(three_pieces(partial_sq), ((0, 5), (0, 0)))
    payload = jnp.concatenate([scaled, pieces], axis=0)
    gathered = lax.all_gather(payload, Z, axis=0, tiled=False)
    half_sq = jnp.sum(gathered[:, part_width : part_width + 3].astype(F32), axis=(0, 1))
    input_sq = half_sq + swapped(half_sq[None])[0]
    row_scale = lax.rsqrt(input_sq / full_width + EPSILON)
    normed = (
        (gathered[:, :part_width].astype(F32) * row_scale).astype(BF16).reshape(half_width, tok_rows)
    )

    chosen = routes.T
    experts = lax.broadcasted_iota(jnp.int32, (groups, tok_rows), 0)
    first_hot = (experts == chosen[0]).astype(F32)
    second_hot = (experts == chosen[1]).astype(F32)
    before = (
        lax.broadcasted_iota(jnp.int32, (tok_rows, tok_rows), 0)
        < lax.broadcasted_iota(jnp.int32, (tok_rows, tok_rows), 1)
    ).astype(BF16)
    earlier = jnp.dot(
        (first_hot + second_hot).astype(BF16), before, preferred_element_type=F32
    )
    first_slot = jnp.sum(earlier * first_hot, axis=0).astype(jnp.int32)
    second_slot = jnp.sum(earlier * second_hot, axis=0).astype(jnp.int32)
    places = lax.broadcasted_iota(jnp.int32, (slots_all, tok_rows), 0)
    first_place = chosen[0] * capacity + first_slot
    second_place = chosen[1] * capacity + second_slot
    first_pick = (places == first_place).astype(BF16)
    second_pick = (places == second_place).astype(BF16)

    outgoing = lax.dot_general(
        first_pick + second_pick, normed, (((1,), (1,)), ((), ())), preferred_element_type=F32
    ).astype(BF16)
    own = lax.all_to_all(
        outgoing.reshape(groups, capacity, half_width), "ep", split_axis=0, concat_axis=0, tiled=True
    ).reshape(slots_all, half_width)
    peer = swapped(own)

    vmem = pl.BlockSpec(memory_space=pltpu.VMEM)
    smem = pl.BlockSpec(memory_space=pltpu.SMEM)
    units = expert_gate.shape[-1]
    width = half_width // pairs
    index = core[None]
    gate = expert_gate.reshape(columns, 2, part_width, units)
    up = expert_up.reshape(columns, 2, part_width, units)
    sent = jax.ShapeDtypeStruct((groups, pairs, capacity, width), BF16)

    def kernel(body, out_shape, *operands):
        return pl.pallas_call(
            body,
            in_specs=[smem] + [vmem] * len(operands),
            out_specs=jax.tree.map(lambda _: vmem, out_shape),
            out_shape=out_shape,
            compiler_params=pltpu.CompilerParams(vmem_limit_bytes=16 * MIB),
            name=body.__name__,
        )(index, *operands)

    gate_pre, up_pre, split_down = kernel(
        own_half_kernel,
        [jax.ShapeDtypeStruct((slots_all, units), F32)] * 2
        + [jax.ShapeDtypeStruct((2, pairs, units, width), BF16)],
        own,
        gate,
        up,
        expert_down.reshape(units, full_width),
    )
    hidden, send = kernel(
        peer_half_kernel,
        [jax.ShapeDtypeStruct((slots_all, units), BF16), sent],
        peer,
        gate_pre,
        up_pre,
        gate,
        up,
        split_down,
    )
    arrived = swapped(send)
    keep = kernel(keep_kernel, sent, hidden, split_down)
    expert_out = (keep.astype(F32) + arrived.astype(F32)).astype(BF16)
    returned = lax.all_to_all(
        expert_out.reshape(groups * pairs, capacity, half_width // pairs),
        ("ep", "zp"),
        split_axis=0,
        concat_axis=0,
        tiled=True,
    ).reshape(pairs * slots_all, half_width // pairs)

    rows = lax.broadcasted_iota(jnp.int32, (pairs * slots_all, tok_rows), 0)
    slot_of_row = rows // (pairs * capacity) * capacity + rows % capacity
    first_back = (slot_of_row == first_place).astype(BF16)
    second_back = (slot_of_row == second_place).astype(BF16)
    contract = (((0,), (0,)), ((), ()))
    first_out = lax.dot_general(returned, first_back, contract, preferred_element_type=F32)
    second_out = lax.dot_general(returned, second_back, contract, preferred_element_type=F32)
    weights = route_weights.T
    partial = (weights[0] * first_out + weights[1] * second_out).astype(BF16)
    parts = lax.all_to_all(
        partial.reshape(columns // pairs, part_width, tok_rows),
        "z8",
        split_axis=0,
        concat_axis=0,
        tiled=True,
    )
    combined = jnp.sum(parts.astype(F32), axis=0)
    output_sq = jnp.sum(sent_to_all(jnp.sum(combined * combined, axis=0)[None], TP), axis=(0, 1))
    result = combined * lax.rsqrt(output_sq / full_width + EPSILON) * post_gain[:, None]
    return result.astype(BF16).T


def solution(mesh):
    torus = Mesh(mesh.devices.reshape(mesh.shape["ep"], 8, 2, 2), ("ep", *TP))
    in_specs = (
        P("ep", TP),
        P(TP),
        P("ep", None, TP),
        P("ep", None, TP),
        P("ep", TP, None),
        P("ep", None),
        P("ep", None),
        P(TP),
    )
    out_specs = P("ep", TP)
    return jax.shard_map(local, mesh=torus, in_specs=in_specs, out_specs=out_specs, check_vma=False)
```

```python
import jax
import jax.numpy as jnp
from jax import lax
from jax.experimental import pallas as pl
from jax.experimental.pallas import tpu as pltpu
from jax.sharding import Mesh
from jax.sharding import PartitionSpec as P

Z = ("z8", "zp")
TP = ("z8", "zp", "core")
EPSILON = 1e-06
F32 = jnp.float32
BF16 = jnp.bfloat16
MIB = 1024 * 1024
VMEM = pl.BlockSpec(memory_space=pltpu.VMEM)
HBM = pl.BlockSpec(memory_space=pltpu.HBM)


def exchanged(value, axis):
    return lax.all_to_all(value, axis, split_axis=0, concat_axis=0, tiled=True)


def swapped(value):
    return lax.ppermute(value, "core", [(0, 1), (1, 0)])


def three_pieces(value):
    high = lax.reduce_precision(value, 8, 7)
    middle = lax.reduce_precision(value - high, 8, 7)
    low = lax.reduce_precision(value - high - middle, 8, 7)
    return jnp.stack([high, middle, low]).astype(BF16)


def in_hbm(value):
    return pltpu.with_memory_space_constraint(value, pltpu.HBM)


def kernel(body, out_shape, *operands, in_specs=None, out_specs=VMEM, scratch_shapes=()):
    return pl.pallas_call(
        body,
        in_specs=in_specs or [VMEM] * len(operands),
        out_specs=out_specs,
        out_shape=out_shape,
        scratch_shapes=scratch_shapes,
        compiler_params=pltpu.CompilerParams(vmem_limit_bytes=16 * MIB),
    )(*operands)


def slots_kernel(chosen, places):
    tok_rows = chosen.shape[1]
    groups = 16
    few = 3 * tok_rows // groups // 2
    experts = lax.broadcasted_iota(jnp.int32, (groups, tok_rows), 0)
    hot = [(experts == chosen[k : k + 1, :]).astype(F32) for k in range(2)]
    before = (
        lax.broadcasted_iota(jnp.int32, (tok_rows, tok_rows), 0)
        < lax.broadcasted_iota(jnp.int32, (tok_rows, tok_rows), 1)
    ).astype(F32)
    earlier = jnp.dot(
        (hot[0] + hot[1]).astype(BF16), before.astype(BF16), preferred_element_type=F32
    )
    for k in range(2):
        slot = jnp.sum(earlier * hot[k], axis=0, keepdims=True).astype(jnp.int32)
        upper = (slot >= few).astype(jnp.int32)
        places[k : k + 1, :] = (
            upper * (groups * few) + chosen[k : k + 1, :] * few + slot - upper * few
        )


def reorder_kernel(down, split_down, held, turned, sems):
    coming = pltpu.make_async_copy(down, held, sems.at[0])
    coming.start()
    size = 512
    row = lax.broadcasted_iota(jnp.int32, (size, size), 0)
    col = lax.broadcasted_iota(jnp.int32, (size, size), 1)
    part = col // 64
    source = (part % 2) * 256 + (part // 2) * 64 + col % 64
    shuffle = (row == source).astype(F32).astype(BF16)
    coming.wait()
    for block in range(held.shape[1] // size):
        value = jnp.dot(
            held[:, block * size : (block + 1) * size], shuffle, preferred_element_type=F32
        ).astype(BF16)
        for part in range(4):
            turned[part, :, block * 128 : block * 128 + 128] = value[
                :, part * 128 : part * 128 + 128
            ]
    leaving = pltpu.make_async_copy(turned, split_down, sems.at[1])
    leaving.start()
    leaving.wait()


def expert_kernel(
    rows, gate_own, up_own, gate_peer, up_peer, down_own, down_peer, sent, *scratch
):
    held, sems = scratch[:-1], scratch[-1]
    copies = [
        pltpu.make_async_copy(source, target, sems.at[k])
        for k, (source, target) in enumerate(
            zip((gate_own, up_own, gate_peer, up_peer, down_own, down_peer), held)
        )
    ]
    for copy in copies:
        copy.start()
    half, units = rows.shape[2], gate_own.shape[-1]
    step = 192
    starts = range(0, rows.shape[1], step)
    hidden = {}
    for which in range(2):
        gate, up = held[2 * which], held[2 * which + 1]
        copies[2 * which].wait()
        copies[2 * which + 1].wait()
        for start in starts:
            here = slice(start, start + step)
            gate_pre = up_pre = None
            for side in range(2):
                value = rows[side, here, :]
                more_gate = jnp.dot(
                    value, gate[:, side].reshape(half, units), preferred_element_type=F32
                )
                more_up = jnp.dot(
                    value, up[:, side].reshape(half, units), preferred_element_type=F32
                )
                gate_pre = more_gate if gate_pre is None else gate_pre + more_gate
                up_pre = more_up if up_pre is None else up_pre + more_up
            hidden[which, start] = (gate_pre / (1.0 + jnp.exp(-gate_pre)) * up_pre).astype(BF16)
    copies[4].wait()
    copies[5].wait()
    for start in starts:
        here = slice(start, start + step)
        for part in range(4):
            out = jnp.dot(hidden[0, start], held[4][part], preferred_element_type=F32)
            out = out + jnp.dot(hidden[1, start], held[5][part], preferred_element_type=F32)
            sent[part, here, :] = out.astype(BF16)


def combine_kernel(returned, places, weights, partial):
    slots_all, tok_rows = returned.shape[1], places.shape[1]
    slots = lax.broadcasted_iota(jnp.int32, (slots_all, tok_rows), 0)
    both = (returned[0].astype(F32) + returned[1].astype(F32)).astype(BF16)
    total = None
    for k in range(2):
        hot = (slots == places[k : k + 1, :]).astype(F32).astype(BF16)
        picked = lax.dot_general(
            both, hot, (((0,), (0,)), ((), ())), preferred_element_type=F32
        )
        picked = picked * weights[k : k + 1, :]
        total = picked if total is None else total + picked
    partial[...] = total.astype(BF16)


def local(tokens, pre_gain, expert_gate, expert_up, expert_down, routes, route_weights, post_gain):
    groups = lax.axis_size("ep")
    columns = lax.axis_size(Z)
    tok_rows, part_width = tokens.shape
    full_width = part_width * lax.axis_size(TP)
    half_width = full_width // 2
    width = full_width // 4
    few = 3 * tok_rows // groups // 2
    slots_all = 2 * groups * few
    units = expert_gate.shape[-1]

    values = tokens.T.astype(F32)
    partial_sq = jnp.sum(values * values, axis=0)
    scaled = (values * pre_gain[:, None]).astype(BF16)
    pieces = jnp.pad(three_pieces(partial_sq), ((0, 5), (0, 0)))
    payload = jnp.concatenate([scaled, pieces], axis=0)
    gathered = lax.all_gather(payload, Z, axis=0, tiled=False)
    half_sq = jnp.sum(gathered[:, part_width : part_width + 3].astype(F32), axis=(0, 1))
    input_sq = half_sq + swapped(half_sq[None])[0]
    row_scale = lax.rsqrt(input_sq / full_width + EPSILON)
    normed = (
        (gathered[:, :part_width].astype(F32) * row_scale).astype(BF16).reshape(half_width, tok_rows)
    )

    places = kernel(slots_kernel, jax.ShapeDtypeStruct((2, tok_rows), jnp.int32), routes.T)
    slots = lax.broadcasted_iota(jnp.int32, (slots_all, tok_rows), 0)
    dispatch = (slots == places[0]).astype(BF16) + (slots == places[1]).astype(BF16)
    outgoing = lax.dot_general(
        dispatch, normed, (((1,), (1,)), ((), ())), preferred_element_type=F32
    ).astype(BF16)
    rows = exchanged(outgoing.reshape(2 * groups, few, half_width), ("core", "ep"))

    gate = expert_gate.reshape(columns, 2, part_width, units)
    up = expert_up.reshape(columns, 2, part_width, units)
    down = kernel(
        reorder_kernel,
        pltpu.HBM((4, units, width), BF16),
        in_hbm(expert_down.reshape(units, full_width)),
        in_specs=[HBM],
        out_specs=HBM,
        scratch_shapes=[
            pltpu.VMEM((units, full_width), BF16),
            pltpu.VMEM((4, units, width), BF16),
            pltpu.SemaphoreType.DMA((2,)),
        ],
    )
    gate_peer = swapped(gate)
    up_peer = swapped(up)
    down_peer = swapped(down)
    sent = kernel(
        expert_kernel,
        jax.ShapeDtypeStruct((4, groups * few, width), BF16),
        rows.reshape(2, groups * few, half_width),
        *(in_hbm(w) for w in (gate, up, gate_peer, up_peer, down, down_peer)),
        in_specs=[VMEM] + [HBM] * 6,
        scratch_shapes=[pltpu.VMEM(gate.shape, BF16)] * 4
        + [pltpu.VMEM(down.shape, BF16)] * 2
        + [pltpu.SemaphoreType.DMA((6,))],
    )
    returned = exchanged(sent.reshape(4 * groups, few, width), ("zp", "core", "ep"))

    partial = kernel(
        combine_kernel,
        jax.ShapeDtypeStruct((width, tok_rows), BF16),
        returned.reshape(2, slots_all, width),
        places,
        route_weights.T,
    )
    parts = exchanged(partial.reshape(columns // 2, part_width, tok_rows), "z8")
    combined = jnp.sum(parts.astype(F32), axis=0)
    own_sq = jnp.sum(combined * combined, axis=0)
    copies = jnp.broadcast_to(own_sq[None, None], (lax.axis_size(TP), 1, tok_rows))
    output_sq = jnp.sum(exchanged(copies, TP), axis=(0, 1))
    result = combined * lax.rsqrt(output_sq / full_width + EPSILON) * post_gain[:, None]
    return result.astype(BF16).T


def solution(mesh):
    torus = Mesh(mesh.devices.reshape(mesh.shape["ep"], 8, 2, 2), ("ep", *TP))
    in_specs = (
        P("ep", TP),
        P(TP),
        P("ep", None, TP),
        P("ep", None, TP),
        P("ep", TP, None),
        P("ep", None),
        P("ep", None),
        P(TP),
    )

    return jax.shard_map(
        local, mesh=torus, in_specs=in_specs, out_specs=P("ep", TP), check_vma=False
    )
```

```python
import jax
import jax.numpy as jnp
from jax import lax
from jax.experimental import pallas as pl
from jax.experimental.pallas import tpu as pltpu
from jax.sharding import Mesh
from jax.sharding import PartitionSpec as P

TP = ("z8", "zp", "core")
EPSILON = 1e-06
F32 = jnp.float32
BF16 = jnp.bfloat16
MIB = 1024 * 1024
VMEM = pl.BlockSpec(memory_space=pltpu.VMEM)
HBM = pl.BlockSpec(memory_space=pltpu.HBM)


def exchanged(value, axis):
    return lax.all_to_all(value, axis, split_axis=0, concat_axis=0, tiled=True)


def swapped(value):
    return lax.ppermute(value, "core", [(0, 1), (1, 0)])


def three_pieces(value):
    high = lax.reduce_precision(value, 8, 7)
    middle = lax.reduce_precision(value - high, 8, 7)
    low = lax.reduce_precision(value - high - middle, 8, 7)
    return jnp.stack([high, middle, low]).astype(BF16)


def in_hbm(value):
    return pltpu.with_memory_space_constraint(value, pltpu.HBM)


def kernel(body, out_shape, *operands, in_specs=None, out_specs=None, scratch_shapes=()):
    return pl.pallas_call(
        body,
        in_specs=in_specs or [VMEM] * len(operands),
        out_specs=out_specs or jax.tree.map(lambda _: VMEM, out_shape),
        out_shape=out_shape,
        scratch_shapes=scratch_shapes,
        compiler_params=pltpu.CompilerParams(vmem_limit_bytes=16 * MIB),
    )(*operands)


def slots_kernel(chosen, places, dispatch):
    slots_all, tok_rows = dispatch.shape
    groups = 16
    few = slots_all // groups // 2
    experts = lax.broadcasted_iota(jnp.int32, (groups, tok_rows), 0)
    hot = [(experts == chosen[k : k + 1, :]).astype(F32) for k in range(2)]
    before = (
        lax.broadcasted_iota(jnp.int32, (tok_rows, tok_rows), 0)
        < lax.broadcasted_iota(jnp.int32, (tok_rows, tok_rows), 1)
    ).astype(F32)
    earlier = jnp.dot(
        (hot[0] + hot[1]).astype(BF16), before.astype(BF16), preferred_element_type=F32
    )
    slots = lax.broadcasted_iota(jnp.int32, (slots_all, tok_rows), 0)
    taken = None
    for k in range(2):
        slot = jnp.sum(earlier * hot[k], axis=0, keepdims=True).astype(jnp.int32)
        upper = (slot >= few).astype(jnp.int32)
        place = upper * (groups * few) + chosen[k : k + 1, :] * few + slot - upper * few
        places[k : k + 1, :] = place
        here = slots == place
        taken = here if taken is None else taken | here
    dispatch[...] = taken.astype(F32).astype(BF16)


def dispatch_kernel(dispatch, gathered, outgoing):
    part_width = 64
    columns, _, tok_rows = gathered.shape
    features = gathered[:, :part_width, :].reshape(columns * part_width, tok_rows)
    value = lax.dot_general(
        dispatch[...], features, (((1,), (1,)), ((), ())), preferred_element_type=F32
    ).astype(BF16)
    outgoing[0] = value
    outgoing[1] = value


def reorder_kernel(down, split_down, held, turned, sems):
    coming = pltpu.make_async_copy(down, held, sems.at[0])
    coming.start()
    size = 512
    row = lax.broadcasted_iota(jnp.int32, (size, size), 0)
    col = lax.broadcasted_iota(jnp.int32, (size, size), 1)
    part = col // 64
    source = (part % 2) * 256 + (part // 2) * 64 + col % 64
    shuffle = (row == source).astype(F32).astype(BF16)
    coming.wait()
    for block in range(held.shape[1] // size):
        value = jnp.dot(
            held[:, block * size : (block + 1) * size], shuffle, preferred_element_type=F32
        ).astype(BF16)
        for part in range(4):
            turned[part, :, block * 128 : block * 128 + 128] = value[
                :, part * 128 : part * 128 + 128
            ]
    leaving = pltpu.make_async_copy(turned, split_down, sems.at[1])
    leaving.start()
    leaving.wait()


def expert_kernel(
    rows, gain, gate_own, up_own, gate_peer, up_peer, down_own, down_peer, sent, *scratch
):
    gates, ups, downs, scaled, sems = scratch
    parts, length, width = rows.shape
    units = gate_own.shape[-1]
    copies = [[], [], []]
    for stage, pairs in enumerate(((gate_own, up_own), (gate_peer, up_peer))):
        for k, (source, target) in enumerate(zip(pairs, (gates, ups))):
            for part in range(parts):
                copies[stage].append(
                    pltpu.make_async_copy(
                        source.at[:, part], target.at[stage, part], sems.at[stage, k, part]
                    )
                )
    for k, source in enumerate((down_own, down_peer)):
        copies[2].append(pltpu.make_async_copy(source, downs.at[k], sems.at[2, k, 0]))
    for stage in copies:
        for copy in stage:
            copy.start()
    step = 192
    starts = range(0, length, step)
    row_scale = {}
    for start in starts:
        here = slice(start, start + step)
        square = None
        for part in range(parts):
            value = rows[part, here, :].astype(F32)
            more = value * value
            square = more if square is None else square + more
            scaled[here, part * width : (part + 1) * width] = (
                value * gain[part : part + 1, :]
            ).astype(BF16)
        mean = jnp.sum(square, axis=1, keepdims=True) / (parts * width)
        row_scale[start] = lax.rsqrt(mean + EPSILON)
    hidden = {}
    for which in range(2):
        for copy in copies[which]:
            copy.wait()
        gate = gates[which].reshape(parts * width, units)
        up = ups[which].reshape(parts * width, units)
        for start in starts:
            value = scaled[start : start + step, :]
            gate_pre = jnp.dot(value, gate, preferred_element_type=F32) * row_scale[start]
            up_pre = jnp.dot(value, up, preferred_element_type=F32) * row_scale[start]
            hidden[which, start] = (gate_pre / (1.0 + jnp.exp(-gate_pre)) * up_pre).astype(BF16)
    for copy in copies[2]:
        copy.wait()
    for start in starts:
        here = slice(start, start + step)
        for part in range(parts):
            out = jnp.dot(hidden[0, start], downs[0, part], preferred_element_type=F32)
            out = out + jnp.dot(hidden[1, start], downs[1, part], preferred_element_type=F32)
            sent[part, here, :] = out.astype(BF16)


def combine_kernel(returned, places, weights, partial):
    slots_all, tok_rows = returned.shape[1], places.shape[1]
    slots = lax.broadcasted_iota(jnp.int32, (slots_all, tok_rows), 0)
    both = (returned[0].astype(F32) + returned[1].astype(F32)).astype(BF16)
    total = None
    for k in range(2):
        hot = (slots == places[k : k + 1, :]).astype(F32).astype(BF16)
        picked = lax.dot_general(
            both, hot, (((0,), (0,)), ((), ())), preferred_element_type=F32
        )
        picked = picked * weights[k : k + 1, :]
        total = picked if total is None else total + picked
    partial[...] = total.astype(BF16)


def local(tokens, pre_gain, expert_gate, expert_up, expert_down, routes, route_weights, post_gain):
    groups = lax.axis_size("ep")
    columns = lax.axis_size("z8")
    tok_rows, part_width = tokens.shape
    full_width = part_width * lax.axis_size(TP)
    width = full_width // 4
    few = 3 * tok_rows // groups // 2
    slots_all = 2 * groups * few
    units = expert_gate.shape[-1]

    pieces = jnp.pad(three_pieces(pre_gain).reshape(1, -1), ((0, 7), (0, tok_rows - 3 * part_width)))
    payload = jnp.concatenate([tokens.T, pieces], axis=0)
    copies = jnp.broadcast_to(payload, (columns, *payload.shape))
    gathered = exchanged(copies, "z8")

    places, dispatch = kernel(
        slots_kernel,
        [
            jax.ShapeDtypeStruct((2, tok_rows), jnp.int32),
            jax.ShapeDtypeStruct((slots_all, tok_rows), BF16),
        ],
        routes.T,
    )
    outgoing = kernel(
        dispatch_kernel, jax.ShapeDtypeStruct((2, slots_all, width), BF16), dispatch, gathered
    )
    rows = exchanged(outgoing.reshape(4 * groups, few, width), ("zp", "core", "ep"))

    gain_pieces = gathered[:, part_width, : 3 * part_width].astype(F32)
    gain = gain_pieces.reshape(columns, 3, part_width).sum(axis=1).reshape(1, width)
    gain = lax.all_gather(gain, ("zp", "core"), axis=0, tiled=True)

    gate = expert_gate.reshape(columns, 4, part_width, units)
    up = expert_up.reshape(columns, 4, part_width, units)
    down = kernel(
        reorder_kernel,
        pltpu.HBM((4, units, width), BF16),
        in_hbm(expert_down.reshape(units, full_width)),
        in_specs=[HBM],
        out_specs=HBM,
        scratch_shapes=[
            pltpu.VMEM((units, full_width), BF16),
            pltpu.VMEM((4, units, width), BF16),
            pltpu.SemaphoreType.DMA((2,)),
        ],
    )
    gate_peer = swapped(gate)
    up_peer = swapped(up)
    down_peer = swapped(down)
    sent = kernel(
        expert_kernel,
        jax.ShapeDtypeStruct((4, groups * few, width), BF16),
        rows.reshape(4, groups * few, width),
        gain,
        *(in_hbm(w) for w in (gate, up, gate_peer, up_peer, down, down_peer)),
        in_specs=[VMEM] * 2 + [HBM] * 6,
        scratch_shapes=[
            pltpu.VMEM((2, 4, columns, part_width, units), BF16),
            pltpu.VMEM((2, 4, columns, part_width, units), BF16),
            pltpu.VMEM((2, 4, units, width), BF16),
            pltpu.VMEM((groups * few, full_width), BF16),
            pltpu.SemaphoreType.DMA((3, 2, 4)),
        ],
    )
    returned = exchanged(sent.reshape(4 * groups, few, width), ("zp", "core", "ep"))

    partial = kernel(
        combine_kernel,
        jax.ShapeDtypeStruct((width, tok_rows), BF16),
        returned.reshape(2, slots_all, width),
        places,
        route_weights.T,
    )
    parts = exchanged(partial.reshape(columns, part_width, tok_rows), "z8")
    combined = jnp.sum(parts.astype(F32), axis=0)
    own_sq = jnp.sum(combined * combined, axis=0)
    copies = jnp.broadcast_to(own_sq[None, None], (lax.axis_size(TP), 1, tok_rows))
    output_sq = jnp.sum(exchanged(copies, TP), axis=(0, 1))
    result = combined * lax.rsqrt(output_sq / full_width + EPSILON) * post_gain[:, None]
    return result.astype(BF16).T


def solution(mesh):
    torus = Mesh(mesh.devices.reshape(mesh.shape["ep"], 8, 2, 2), ("ep", *TP))
    in_specs = (
        P("ep", TP),
        P(TP),
        P("ep", None, TP),
        P("ep", None, TP),
        P("ep", TP, None),
        P("ep", None),
        P("ep", None),
        P(TP),
    )

    return jax.shard_map(
        local, mesh=torus, in_specs=in_specs, out_specs=P("ep", TP), check_vma=False
    )
```

```python
import jax
import jax.numpy as jnp
from jax import lax
from jax.experimental import pallas as pl
from jax.experimental.pallas import tpu as pltpu
from jax.sharding import Mesh
from jax.sharding import PartitionSpec as P

TP = ("z8", "zp", "core")
EPSILON = 1e-06
F32 = jnp.float32
BF16 = jnp.bfloat16
MIB = 1024 * 1024
VMEM = pl.BlockSpec(memory_space=pltpu.VMEM)
HBM = pl.BlockSpec(memory_space=pltpu.HBM)
ANY = pl.BlockSpec(memory_space=pl.ANY)


def exchanged(value, axis):
    return lax.all_to_all(value, axis, split_axis=0, concat_axis=0, tiled=True)


def swapped(value):
    return lax.ppermute(value, "core", [(0, 1), (1, 0)])


def in_hbm(value):
    return pltpu.with_memory_space_constraint(value, pltpu.HBM)


def kernel(body, out_shape, *operands, in_specs=None, out_specs=None, scratch_shapes=()):
    return pl.pallas_call(
        body,
        in_specs=in_specs or [VMEM] * len(operands),
        out_specs=out_specs or jax.tree.map(lambda _: VMEM, out_shape),
        out_shape=out_shape,
        scratch_shapes=scratch_shapes,
        compiler_params=pltpu.CompilerParams(vmem_limit_bytes=16 * MIB),
    )(*operands)


def spread_kernel(tokens, gain, copies, payload, sems):
    part_width, lanes = tokens.shape[0], payload.shape[1]
    payload[0:part_width, :] = tokens[:, :lanes]
    payload[part_width : 2 * part_width, :] = tokens[:, lanes:]
    value = gain[...]
    high = value.astype(BF16).astype(F32)
    middle = (value - high).astype(BF16).astype(F32)
    low = value - high - middle
    row = lax.broadcasted_iota(jnp.int32, (8, lanes), 0)
    picked = jnp.where(row == 0, high, jnp.where(row == 1, middle, jnp.where(row == 2, low, 0.0)))
    payload[2 * part_width :, :] = picked.astype(BF16)
    leaving = [
        pltpu.make_async_copy(payload, copies.at[k], sems.at[k]) for k in range(copies.shape[0])
    ]
    for copy in leaving:
        copy.start()
    for copy in leaving:
        copy.wait()


def slots_kernel(chosen, places, dispatch):
    slots_all, tok_rows = dispatch.shape
    groups = 16
    few = slots_all // groups // 2
    experts = lax.broadcasted_iota(jnp.int32, (groups, tok_rows), 0)
    hot = [(experts == chosen[k : k + 1, :]).astype(F32) for k in range(2)]
    before = (
        lax.broadcasted_iota(jnp.int32, (tok_rows, tok_rows), 0)
        < lax.broadcasted_iota(jnp.int32, (tok_rows, tok_rows), 1)
    ).astype(F32)
    earlier = jnp.dot(
        (hot[0] + hot[1]).astype(BF16), before.astype(BF16), preferred_element_type=F32
    )
    slots = lax.broadcasted_iota(jnp.int32, (slots_all, tok_rows), 0)
    taken = None
    for k in range(2):
        slot = jnp.sum(earlier * hot[k], axis=0, keepdims=True).astype(jnp.int32)
        upper = (slot >= few).astype(jnp.int32)
        place = upper * (groups * few) + chosen[k : k + 1, :] * few + slot - upper * few
        places[k : k + 1, :] = place
        here = slots == place
        taken = here if taken is None else taken | here
    dispatch[...] = taken.astype(F32).astype(BF16)


def dispatch_kernel(dispatch, gathered, outgoing, held, sems):
    part_width = 64
    lower = gathered[:, :part_width, :]
    upper = gathered[:, part_width : 2 * part_width, :]
    features = jnp.concatenate([lower, upper], axis=2).reshape(-1, 2 * gathered.shape[2])
    length = dispatch.shape[0]
    step = length // 4
    leaving = []
    for k in range(4):
        here = pl.ds(k * step, step)
        held[here, :] = lax.dot_general(
            dispatch[here, :], features, (((1,), (1,)), ((), ())), preferred_element_type=F32
        ).astype(BF16)
        for pair in range(2):
            copy = pltpu.make_async_copy(
                held.at[here], outgoing.at[pair, here], sems.at[pair, k]
            )
            copy.start()
            leaving.append(copy)
    for copy in leaving:
        copy.wait()


def reorder_kernel(down, split_down, held, turned, sems):
    coming = pltpu.make_async_copy(down, held, sems.at[0])
    coming.start()
    size = 512
    row = lax.broadcasted_iota(jnp.int32, (size, size), 0)
    col = lax.broadcasted_iota(jnp.int32, (size, size), 1)
    part = col // 64
    source = (part % 2) * 256 + (part // 2) * 64 + col % 64
    shuffle = (row == source).astype(F32).astype(BF16)
    coming.wait()
    for block in range(held.shape[1] // size):
        value = jnp.dot(
            held[:, block * size : (block + 1) * size], shuffle, preferred_element_type=F32
        ).astype(BF16)
        for part in range(4):
            turned[part, :, block * 128 : block * 128 + 128] = value[
                :, part * 128 : part * 128 + 128
            ]
    leaving = pltpu.make_async_copy(turned, split_down, sems.at[1])
    leaving.start()
    leaving.wait()


def expert_kernel(
    rows, gain, gate_own, up_own, gate_peer, up_peer, down_own, down_peer, sent, *scratch
):
    gates, ups, downs, scaled, sems = scratch
    parts, length, width = rows.shape
    units = gate_own.shape[-1]
    copies = [[], [], []]
    for stage, pairs in enumerate(((gate_own, up_own), (gate_peer, up_peer))):
        for k, (source, target) in enumerate(zip(pairs, (gates, ups))):
            for part in range(parts):
                copies[stage].append(
                    pltpu.make_async_copy(
                        source.at[:, part], target.at[stage, part], sems.at[stage, k, part]
                    )
                )
    for k, source in enumerate((down_own, down_peer)):
        copies[2].append(pltpu.make_async_copy(source, downs.at[k], sems.at[2, k, 0]))
    for stage in copies:
        for copy in stage:
            copy.start()
    step = 192
    starts = range(0, length, step)
    row_scale = {}
    for start in starts:
        here = slice(start, start + step)
        square = None
        for part in range(parts):
            value = rows[part, here, :].astype(F32)
            more = value * value
            square = more if square is None else square + more
            scaled[here, part * width : (part + 1) * width] = (
                value * gain[part : part + 1, :]
            ).astype(BF16)
        mean = jnp.sum(square, axis=1, keepdims=True) / (parts * width)
        row_scale[start] = lax.rsqrt(mean + EPSILON)
    hidden = {}
    for which in range(2):
        for copy in copies[which]:
            copy.wait()
        gate = gates[which].reshape(parts * width, units)
        up = ups[which].reshape(parts * width, units)
        for start in starts:
            value = scaled[start : start + step, :]
            gate_pre = jnp.dot(value, gate, preferred_element_type=F32) * row_scale[start]
            up_pre = jnp.dot(value, up, preferred_element_type=F32) * row_scale[start]
            hidden[which, start] = (gate_pre / (1.0 + jnp.exp(-gate_pre)) * up_pre).astype(BF16)
    for copy in copies[2]:
        copy.wait()
    for start in starts:
        here = slice(start, start + step)
        for part in range(parts):
            out = jnp.dot(hidden[0, start], downs[0, part], preferred_element_type=F32)
            out = out + jnp.dot(hidden[1, start], downs[1, part], preferred_element_type=F32)
            sent[part, here, :] = out.astype(BF16)


def combine_kernel(returned, places, weights, partial):
    slots_all, tok_rows = returned.shape[1], places.shape[1]
    slots = lax.broadcasted_iota(jnp.int32, (slots_all, tok_rows), 0)
    both = (returned[0].astype(F32) + returned[1].astype(F32)).astype(BF16)
    total = None
    for k in range(2):
        hot = (slots == places[k : k + 1, :]).astype(F32).astype(BF16)
        picked = lax.dot_general(
            both, hot, (((0,), (0,)), ((), ())), preferred_element_type=F32
        )
        picked = picked * weights[k : k + 1, :]
        total = picked if total is None else total + picked
    partial[...] = total.astype(BF16)


def local(tokens, pre_gain, expert_gate, expert_up, expert_down, routes, route_weights, post_gain):
    groups = lax.axis_size("ep")
    columns = lax.axis_size("z8")
    tok_rows, part_width = tokens.shape
    full_width = part_width * lax.axis_size(TP)
    width = full_width // 4
    few = 3 * tok_rows // groups // 2
    slots_all = 2 * groups * few
    units = expert_gate.shape[-1]

    lanes = tok_rows // 2
    copies = kernel(
        spread_kernel,
        pltpu.HBM((columns, 2 * part_width + 8, lanes), BF16),
        tokens.T,
        jnp.pad(pre_gain[None], ((0, 0), (0, lanes - part_width))),
        out_specs=HBM,
        scratch_shapes=[
            pltpu.VMEM((2 * part_width + 8, lanes), BF16),
            pltpu.SemaphoreType.DMA((columns,)),
        ],
    )
    gathered = exchanged(copies, "z8")

    places, dispatch = kernel(
        slots_kernel,
        [
            jax.ShapeDtypeStruct((2, tok_rows), jnp.int32),
            jax.ShapeDtypeStruct((slots_all, tok_rows), BF16),
        ],
        routes.T,
    )
    outgoing = kernel(
        dispatch_kernel,
        pltpu.HBM((2, slots_all, width), BF16),
        dispatch,
        gathered,
        out_specs=HBM,
        scratch_shapes=[pltpu.VMEM((slots_all, width), BF16), pltpu.SemaphoreType.DMA((2, 4))],
    )
    rows = exchanged(outgoing.reshape(4 * groups, few, width), ("zp", "core", "ep"))

    gain = gathered[:, 2 * part_width : 2 * part_width + 3, :part_width].astype(F32)
    gain = gain.sum(axis=1).reshape(1, width)
    gain = lax.all_gather(gain, ("zp", "core"), axis=0, tiled=True)

    gate = expert_gate.reshape(columns, 4, part_width, units)
    up = expert_up.reshape(columns, 4, part_width, units)
    down = kernel(
        reorder_kernel,
        pltpu.HBM((4, units, width), BF16),
        in_hbm(expert_down.reshape(units, full_width)),
        in_specs=[HBM],
        out_specs=HBM,
        scratch_shapes=[
            pltpu.VMEM((units, full_width), BF16),
            pltpu.VMEM((4, units, width), BF16),
            pltpu.SemaphoreType.DMA((2,)),
        ],
    )
    gate_peer = swapped(gate)
    up_peer = swapped(up)
    down_peer = swapped(down)
    sent = kernel(
        expert_kernel,
        jax.ShapeDtypeStruct((4, groups * few, width), BF16),
        rows.reshape(4, groups * few, width),
        gain,
        in_hbm(gate),
        in_hbm(up),
        gate_peer,
        in_hbm(up_peer),
        in_hbm(down),
        in_hbm(down_peer),
        in_specs=[VMEM] * 2 + [HBM] * 2 + [ANY] + [HBM] * 3,
        scratch_shapes=[
            pltpu.VMEM((2, 4, columns, part_width, units), BF16),
            pltpu.VMEM((2, 4, columns, part_width, units), BF16),
            pltpu.VMEM((2, 4, units, width), BF16),
            pltpu.VMEM((groups * few, full_width), BF16),
            pltpu.SemaphoreType.DMA((3, 2, 4)),
        ],
    )
    returned = exchanged(sent.reshape(4 * groups, few, width), ("zp", "core", "ep"))

    partial = kernel(
        combine_kernel,
        jax.ShapeDtypeStruct((width, tok_rows), BF16),
        returned.reshape(2, slots_all, width),
        places,
        route_weights.T,
    )
    parts = exchanged(partial.reshape(columns, part_width, tok_rows), "z8")
    combined = jnp.sum(parts.astype(F32), axis=0)
    own_sq = jnp.sum(combined * combined, axis=0)
    copies = jnp.broadcast_to(own_sq[None, None], (lax.axis_size(TP), 1, tok_rows))
    output_sq = jnp.sum(exchanged(copies, TP), axis=(0, 1))
    result = combined * lax.rsqrt(output_sq / full_width + EPSILON) * post_gain[:, None]
    return result.astype(BF16).T


def solution(mesh):
    torus = Mesh(mesh.devices.reshape(mesh.shape["ep"], 8, 2, 2), ("ep", *TP))
    in_specs = (
        P("ep", TP),
        P(TP),
        P("ep", None, TP),
        P("ep", None, TP),
        P("ep", TP, None),
        P("ep", None),
        P("ep", None),
        P(TP),
    )

    return jax.shard_map(
        local, mesh=torus, in_specs=in_specs, out_specs=P("ep", TP), check_vma=False
    )
```

```python
import jax
import jax.numpy as jnp
from jax import lax
from jax.experimental import pallas as pl
from jax.experimental.pallas import tpu as pltpu
from jax.sharding import Mesh
from jax.sharding import PartitionSpec as P

TP = ("z8", "zp", "core")
EPSILON = 1e-06
F32 = jnp.float32
BF16 = jnp.bfloat16
MIB = 1024 * 1024
VMEM = pl.BlockSpec(memory_space=pltpu.VMEM)
HBM = pl.BlockSpec(memory_space=pltpu.HBM)
ANY = pl.BlockSpec(memory_space=pl.ANY)


def exchanged(value, axis):
    return lax.all_to_all(value, axis, split_axis=0, concat_axis=0, tiled=True)


def swapped(value):
    return lax.ppermute(value, "core", [(0, 1), (1, 0)])


def in_hbm(value):
    return pltpu.with_memory_space_constraint(value, pltpu.HBM)


def kernel(body, out_shape, *operands, in_specs=None, out_specs=None, scratch_shapes=()):
    return pl.pallas_call(
        body,
        in_specs=in_specs or [VMEM] * len(operands),
        out_specs=out_specs or jax.tree.map(lambda _: VMEM, out_shape),
        out_shape=out_shape,
        scratch_shapes=scratch_shapes,
        compiler_params=pltpu.CompilerParams(vmem_limit_bytes=16 * MIB),
    )(*operands)


def spread_kernel(
    tokens_hbm, gain_hbm, chosen_hbm, copies, places, dispatch, tokens, gain, chosen, payload, in_sems
):
    coming = [
        pltpu.make_async_copy(tokens_hbm, tokens, in_sems.at[0]),
        pltpu.make_async_copy(gain_hbm, gain, in_sems.at[1]),
        pltpu.make_async_copy(chosen_hbm, chosen, in_sems.at[2]),
    ]
    for copy in coming:
        copy.start()
    for copy in coming:
        copy.wait()
    part_width, lanes = tokens.shape[0], payload.shape[1]
    payload[0:part_width, :] = tokens[:, :lanes]
    payload[part_width : 2 * part_width, :] = tokens[:, lanes:]
    value = jnp.concatenate([gain[...], jnp.zeros_like(gain)], axis=1)
    high = value.astype(BF16).astype(F32)
    middle = (value - high).astype(BF16).astype(F32)
    low = value - high - middle
    row = lax.broadcasted_iota(jnp.int32, (8, lanes), 0)
    picked = jnp.where(row == 0, high, jnp.where(row == 1, middle, jnp.where(row == 2, low, 0.0)))
    payload[2 * part_width :, :] = picked.astype(BF16)
    for k in range(copies.shape[0]):
        copies[k] = payload[...]
    number_slots(chosen, places, dispatch)


def number_slots(chosen, places, dispatch):
    slots_all, tok_rows = dispatch.shape
    groups = 16
    few = slots_all // groups // 2
    experts = lax.broadcasted_iota(jnp.int32, (groups, tok_rows), 0)
    hot = [(experts == chosen[k : k + 1, :]).astype(F32) for k in range(2)]
    before = (
        lax.broadcasted_iota(jnp.int32, (tok_rows, tok_rows), 0)
        < lax.broadcasted_iota(jnp.int32, (tok_rows, tok_rows), 1)
    ).astype(F32)
    earlier = jnp.dot(
        (hot[0] + hot[1]).astype(BF16), before.astype(BF16), preferred_element_type=F32
    )
    slots = lax.broadcasted_iota(jnp.int32, (slots_all, tok_rows), 0)
    taken = None
    for k in range(2):
        slot = jnp.sum(earlier * hot[k], axis=0, keepdims=True).astype(jnp.int32)
        upper = (slot >= few).astype(jnp.int32)
        place = upper * (groups * few) + chosen[k : k + 1, :] * few + slot - upper * few
        places[k : k + 1, :] = place
        here = slots == place
        taken = here if taken is None else taken | here
    dispatch[...] = taken.astype(F32).astype(BF16)


def dispatch_kernel(dispatch, gathered, outgoing, held, sems):
    part_width = 64
    lower = gathered[:, :part_width, :]
    upper = gathered[:, part_width : 2 * part_width, :]
    width = gathered.shape[0] * part_width
    lower = lower.reshape(width, -1).astype(F32).T.astype(BF16)
    upper = upper.reshape(width, -1).astype(F32).T.astype(BF16)
    features = jnp.concatenate([lower, upper], axis=0)
    length = dispatch.shape[0]
    step = length // 4
    leaving = []
    for k in range(4):
        here = pl.ds(k * step, step)
        held[here, :] = jnp.dot(
            dispatch[here, :], features, preferred_element_type=F32
        ).astype(BF16)
        for pair in range(2):
            copy = pltpu.make_async_copy(
                held.at[here], outgoing.at[pair, here], sems.at[pair, k]
            )
            copy.start()
            leaving.append(copy)
    for copy in leaving:
        copy.wait()


def reorder_kernel(down, split_down, held, turned, sems):
    coming = pltpu.make_async_copy(down, held, sems.at[0])
    coming.start()
    size = 512
    row = lax.broadcasted_iota(jnp.int32, (size, size), 0)
    col = lax.broadcasted_iota(jnp.int32, (size, size), 1)
    part = col // 64
    source = (part % 2) * 256 + (part // 2) * 64 + col % 64
    shuffle = (row == source).astype(F32).astype(BF16)
    coming.wait()
    for block in range(held.shape[1] // size):
        value = jnp.dot(
            held[:, block * size : (block + 1) * size], shuffle, preferred_element_type=F32
        ).astype(BF16)
        for part in range(4):
            turned[part, :, block * 128 : block * 128 + 128] = value[
                :, part * 128 : part * 128 + 128
            ]
    leaving = pltpu.make_async_copy(turned, split_down, sems.at[1])
    leaving.start()
    leaving.wait()


def expert_kernel(
    rows, gain, gate_own, up_own, gate_peer, up_peer, down_own, down_peer, sent, *scratch
):
    held_up_peer, held_gate, held_up, down_first, down_second, scaled, sems = scratch
    parts, length, width = rows.shape
    units = gate_own.shape[-1]
    copies = [
        pltpu.make_async_copy(source, target, sems.at[k])
        for k, (source, target) in enumerate(
            (
                (up_peer, held_up_peer),
                (gate_own, held_gate),
                (up_own, held_up),
                (down_peer, down_first),
                (down_own, down_second),
            )
        )
    ]
    for copy in copies:
        copy.start()
    step = 192
    starts = range(0, length, step)

    def product(start, weight):
        total = None
        for part in range(parts):
            value = scaled[start : start + step, part * width : (part + 1) * width]
            more = jnp.dot(
                value, weight[:, part].reshape(width, units), preferred_element_type=F32
            )
            total = more if total is None else total + more
        return total * row_scale[start]

    row_scale = {}
    gate_pre = {}
    for start in starts:
        here = slice(start, start + step)
        square = None
        for part in range(parts):
            value = rows[part, here, :].astype(F32)
            more = value * value
            square = more if square is None else square + more
            scaled[here, part * width : (part + 1) * width] = (
                value * gain[part : part + 1, :]
            ).astype(BF16)
        mean = jnp.sum(square, axis=1, keepdims=True) / (parts * width)
        row_scale[start] = lax.rsqrt(mean + EPSILON)
        gate_pre[start] = product(start, gate_peer)
    hidden = {}
    copies[0].wait()
    for start in starts:
        value = gate_pre[start]
        up_pre = product(start, held_up_peer)
        hidden[0, start] = (value / (1.0 + jnp.exp(-value)) * up_pre).astype(BF16)
    copies[1].wait()
    for start in starts:
        gate_pre[start] = product(start, held_gate)
    copies[2].wait()
    for start in starts:
        value = gate_pre[start]
        up_pre = product(start, held_up)
        hidden[1, start] = (value / (1.0 + jnp.exp(-value)) * up_pre).astype(BF16)
    copies[3].wait()
    copies[4].wait()
    for start in starts:
        here = slice(start, start + step)
        for part in range(parts):
            out = jnp.dot(hidden[0, start], down_first[part], preferred_element_type=F32)
            out = out + jnp.dot(hidden[1, start], down_second[part], preferred_element_type=F32)
            sent[part, here, :] = out.astype(BF16)


def combine_kernel(returned, places, weights, partial):
    slots_all, tok_rows = returned.shape[1], places.shape[1]
    slots = lax.broadcasted_iota(jnp.int32, (slots_all, tok_rows), 0)
    both = (returned[0].astype(F32) + returned[1].astype(F32)).astype(BF16)
    total = None
    for k in range(2):
        hot = (slots == places[k : k + 1, :]).astype(F32).astype(BF16)
        picked = lax.dot_general(
            both, hot, (((0,), (0,)), ((), ())), preferred_element_type=F32
        )
        picked = picked * weights[k : k + 1, :]
        total = picked if total is None else total + picked
    partial[...] = total.astype(BF16)


def local(tokens, pre_gain, expert_gate, expert_up, expert_down, routes, route_weights, post_gain):
    groups = lax.axis_size("ep")
    columns = lax.axis_size("z8")
    tok_rows, part_width = tokens.shape
    full_width = part_width * lax.axis_size(TP)
    width = full_width // 4
    few = 3 * tok_rows // groups // 2
    slots_all = 2 * groups * few
    units = expert_gate.shape[-1]

    lanes = tok_rows // 2
    copies, places, dispatch = kernel(
        spread_kernel,
        [
            jax.ShapeDtypeStruct((columns, 2 * part_width + 8, lanes), BF16),
            jax.ShapeDtypeStruct((2, tok_rows), jnp.int32),
            jax.ShapeDtypeStruct((slots_all, tok_rows), BF16),
        ],
        in_hbm(tokens.T),
        in_hbm(pre_gain[None]),
        in_hbm(routes.T),
        in_specs=[HBM] * 3,
        scratch_shapes=[
            pltpu.VMEM((part_width, tok_rows), BF16),
            pltpu.VMEM((1, part_width), F32),
            pltpu.VMEM((2, tok_rows), jnp.int32),
            pltpu.VMEM((2 * part_width + 8, lanes), BF16),
            pltpu.SemaphoreType.DMA((3,)),
        ],
    )
    gathered = exchanged(copies, "z8")

    outgoing = kernel(
        dispatch_kernel,
        pltpu.HBM((2, slots_all, width), BF16),
        dispatch,
        gathered,
        out_specs=HBM,
        scratch_shapes=[pltpu.VMEM((slots_all, width), BF16), pltpu.SemaphoreType.DMA((2, 4))],
    )
    rows = exchanged(outgoing.reshape(4 * groups, few, width), ("zp", "core", "ep"))

    gain = gathered[:, 2 * part_width : 2 * part_width + 3, :part_width].astype(F32)
    gain = gain.sum(axis=1).reshape(1, width)
    gain = lax.all_gather(gain, ("zp", "core"), axis=0, tiled=True)

    gate = expert_gate.reshape(columns, 4, part_width, units)
    up = expert_up.reshape(columns, 4, part_width, units)
    down = kernel(
        reorder_kernel,
        pltpu.HBM((4, units, width), BF16),
        in_hbm(expert_down.reshape(units, full_width)),
        in_specs=[HBM],
        out_specs=HBM,
        scratch_shapes=[
            pltpu.VMEM((units, full_width), BF16),
            pltpu.VMEM((4, units, width), BF16),
            pltpu.SemaphoreType.DMA((2,)),
        ],
    )
    gate_peer = swapped(gate)
    up_peer = swapped(up)
    down_peer = swapped(down)
    sent = kernel(
        expert_kernel,
        jax.ShapeDtypeStruct((4, groups * few, width), BF16),
        rows.reshape(4, groups * few, width),
        gain,
        in_hbm(gate),
        in_hbm(up),
        gate_peer,
        in_hbm(up_peer),
        in_hbm(down),
        in_hbm(down_peer),
        in_specs=[VMEM] * 2 + [HBM] * 2 + [VMEM] + [HBM] * 3,
        scratch_shapes=[pltpu.VMEM(gate.shape, BF16)] * 3
        + [pltpu.VMEM(down.shape, BF16)] * 2
        + [pltpu.VMEM((groups * few, full_width), BF16), pltpu.SemaphoreType.DMA((5,))],
    )
    returned = exchanged(sent.reshape(4 * groups, few, width), ("zp", "core", "ep"))

    partial = kernel(
        combine_kernel,
        jax.ShapeDtypeStruct((width, tok_rows), BF16),
        returned.reshape(2, slots_all, width),
        places,
        route_weights.T,
    )
    parts = exchanged(partial.reshape(columns, part_width, tok_rows), "z8")
    combined = jnp.sum(parts.astype(F32), axis=0)
    own_sq = jnp.sum(combined * combined, axis=0)
    copies = jnp.broadcast_to(own_sq[None, None], (lax.axis_size(TP), 1, tok_rows))
    output_sq = jnp.sum(exchanged(copies, TP), axis=(0, 1))
    result = combined * lax.rsqrt(output_sq / full_width + EPSILON) * post_gain[:, None]
    return result.astype(BF16).T


def solution(mesh):
    torus = Mesh(mesh.devices.reshape(mesh.shape["ep"], 8, 2, 2), ("ep", *TP))
    in_specs = (
        P("ep", TP),
        P(TP),
        P("ep", None, TP),
        P("ep", None, TP),
        P("ep", TP, None),
        P("ep", None),
        P("ep", None),
        P(TP),
    )

    return jax.shard_map(
        local, mesh=torus, in_specs=in_specs, out_specs=P("ep", TP), check_vma=False
    )
```

```python
import jax
import jax.numpy as jnp
from jax import lax
from jax.experimental import pallas as pl
from jax.experimental.pallas import tpu as pltpu
from jax.sharding import Mesh
from jax.sharding import PartitionSpec as P

TP = ("z8", "zp", "core")
EPSILON = 1e-06
F32 = jnp.float32
BF16 = jnp.bfloat16
MIB = 1024 * 1024
VMEM = pl.BlockSpec(memory_space=pltpu.VMEM)
HBM = pl.BlockSpec(memory_space=pltpu.HBM)
ANY = pl.BlockSpec(memory_space=pl.ANY)


def exchanged(value, axis):
    return lax.all_to_all(value, axis, split_axis=0, concat_axis=0, tiled=True)


def swapped(value):
    return lax.ppermute(value, "core", [(0, 1), (1, 0)])


def in_hbm(value):
    return pltpu.with_memory_space_constraint(value, pltpu.HBM)


def kernel(body, out_shape, *operands, in_specs=None, out_specs=None, scratch_shapes=()):
    return pl.pallas_call(
        body,
        in_specs=in_specs or [VMEM] * len(operands),
        out_specs=out_specs or jax.tree.map(lambda _: VMEM, out_shape),
        out_shape=out_shape,
        scratch_shapes=scratch_shapes,
        compiler_params=pltpu.CompilerParams(vmem_limit_bytes=16 * MIB),
    )(*operands)


def spread_kernel(
    tokens_hbm, gain_hbm, chosen_hbm, copies, places, dispatch, tokens, gain, chosen, payload, in_sems
):
    coming = [
        pltpu.make_async_copy(tokens_hbm, tokens, in_sems.at[0]),
        pltpu.make_async_copy(gain_hbm, gain, in_sems.at[1]),
        pltpu.make_async_copy(chosen_hbm, chosen, in_sems.at[2]),
    ]
    for copy in coming:
        copy.start()
    for copy in coming:
        copy.wait()
    part_width, lanes = tokens.shape[0], payload.shape[1]
    payload[0:part_width, :] = tokens[:, :lanes]
    payload[part_width : 2 * part_width, :] = tokens[:, lanes:]
    value = jnp.concatenate([gain[...], jnp.zeros_like(gain)], axis=1)
    high = value.astype(BF16).astype(F32)
    middle = (value - high).astype(BF16).astype(F32)
    low = value - high - middle
    row = lax.broadcasted_iota(jnp.int32, (8, lanes), 0)
    picked = jnp.where(row == 0, high, jnp.where(row == 1, middle, jnp.where(row == 2, low, 0.0)))
    payload[2 * part_width :, :] = picked.astype(BF16)
    for k in range(copies.shape[0]):
        copies[k] = payload[...]
    number_slots(chosen, places, dispatch)


def number_slots(chosen, places, dispatch):
    slots_all, tok_rows = dispatch.shape
    groups = 16
    few = slots_all // groups // 2
    experts = lax.broadcasted_iota(jnp.int32, (groups, tok_rows), 0)
    hot = [(experts == chosen[k : k + 1, :]).astype(F32) for k in range(2)]
    before = (
        lax.broadcasted_iota(jnp.int32, (tok_rows, tok_rows), 0)
        < lax.broadcasted_iota(jnp.int32, (tok_rows, tok_rows), 1)
    ).astype(F32)
    earlier = jnp.dot(
        (hot[0] + hot[1]).astype(BF16), before.astype(BF16), preferred_element_type=F32
    )
    slots = lax.broadcasted_iota(jnp.int32, (slots_all, tok_rows), 0)
    taken = None
    for k in range(2):
        slot = jnp.sum(earlier * hot[k], axis=0, keepdims=True).astype(jnp.int32)
        upper = (slot >= few).astype(jnp.int32)
        place = upper * (groups * few) + chosen[k : k + 1, :] * few + slot - upper * few
        places[k : k + 1, :] = place
        here = slots == place
        taken = here if taken is None else taken | here
    dispatch[...] = taken.astype(F32).astype(BF16)


def dispatch_kernel(dispatch, gathered, outgoing, held, sems):
    part_width = 64
    lower = gathered[:, :part_width, :]
    upper = gathered[:, part_width : 2 * part_width, :]
    width = gathered.shape[0] * part_width
    lower = lower.reshape(width, -1).astype(F32).T.astype(BF16)
    upper = upper.reshape(width, -1).astype(F32).T.astype(BF16)
    features = jnp.concatenate([lower, upper], axis=0)
    length = dispatch.shape[0]
    step = length // 4
    leaving = []
    for k in range(4):
        here = pl.ds(k * step, step)
        held[here, :] = jnp.dot(
            dispatch[here, :], features, preferred_element_type=F32
        ).astype(BF16)
        for pair in range(2):
            copy = pltpu.make_async_copy(
                held.at[here], outgoing.at[pair, here], sems.at[pair, k]
            )
            copy.start()
            leaving.append(copy)
    for copy in leaving:
        copy.wait()


def reorder_kernel(down, gate, split_down, gate_head, held, turned, sems):
    coming = pltpu.make_async_copy(down, held, sems.at[0])
    coming.start()
    keeping = pltpu.make_async_copy(gate.at[0 : gate_head.shape[0]], gate_head, sems.at[2])
    keeping.start()
    size = 512
    row = lax.broadcasted_iota(jnp.int32, (size, size), 0)
    col = lax.broadcasted_iota(jnp.int32, (size, size), 1)
    part = col // 64
    source = (part % 2) * 256 + (part // 2) * 64 + col % 64
    shuffle = (row == source).astype(F32).astype(BF16)
    coming.wait()
    for block in range(held.shape[1] // size):
        value = jnp.dot(
            held[:, block * size : (block + 1) * size], shuffle, preferred_element_type=F32
        ).astype(BF16)
        for part in range(4):
            turned[part, :, block * 128 : block * 128 + 128] = value[
                :, part * 128 : part * 128 + 128
            ]
    leaving = pltpu.make_async_copy(turned, split_down, sems.at[1])
    leaving.start()
    leaving.wait()
    keeping.wait()


def expert_kernel(
    rows, gain, head, gate_own, up_own, gate_peer, up_peer, down_own, down_peer, sent, *scratch
):
    held_up_peer, held_gate, held_up, down_first, down_second, scaled, sems = scratch
    parts, length, width = rows.shape
    units = gate_own.shape[-1]
    kept = head.shape[0]
    copies = [
        pltpu.make_async_copy(source, target, sems.at[k])
        for k, (source, target) in enumerate(
            (
                (gate_own.at[kept:], held_gate.at[kept:]),
                (up_peer, held_up_peer),
                (up_own, held_up),
                (down_peer, down_first),
                (down_own, down_second),
            )
        )
    ]
    for k, copy in enumerate(copies):
        copy.start(priority=k // 3)
    step = 192
    starts = range(0, length, step)

    def product(start, weight):
        total = None
        for part in range(parts):
            value = scaled[start : start + step, part * width : (part + 1) * width]
            more = jnp.dot(
                value, weight[:, part].reshape(width, units), preferred_element_type=F32
            )
            total = more if total is None else total + more
        return total * row_scale[start]

    row_scale = {}
    gate_pre = {}
    for start in starts:
        here = slice(start, start + step)
        square = None
        for part in range(parts):
            value = rows[part, here, :].astype(F32)
            more = value * value
            square = more if square is None else square + more
            scaled[here, part * width : (part + 1) * width] = (
                value * gain[part : part + 1, :]
            ).astype(BF16)
        mean = jnp.sum(square, axis=1, keepdims=True) / (parts * width)
        row_scale[start] = lax.rsqrt(mean + EPSILON)
        gate_pre[start] = product(start, gate_peer)
    held_gate[0:kept] = head[...]
    copies[0].wait()
    own_pre = {start: product(start, held_gate) for start in starts}
    hidden = {}
    for k, (pre, weight) in enumerate(((gate_pre, held_up_peer), (own_pre, held_up))):
        copies[1 + k].wait()
        for start in starts:
            value = pre[start]
            up_pre = product(start, weight)
            hidden[k, start] = (value / (1.0 + jnp.exp(-value)) * up_pre).astype(BF16)
    copies[3].wait()
    copies[4].wait()
    for start in starts:
        here = slice(start, start + step)
        for part in range(parts):
            out = jnp.dot(hidden[0, start], down_first[part], preferred_element_type=F32)
            out = out + jnp.dot(hidden[1, start], down_second[part], preferred_element_type=F32)
            sent[part, here, :] = out.astype(BF16)


def combine_kernel(returned, places, weights, partial):
    slots_all, tok_rows = returned.shape[1], places.shape[1]
    slots = lax.broadcasted_iota(jnp.int32, (slots_all, tok_rows), 0)
    both = (returned[0].astype(F32) + returned[1].astype(F32)).astype(BF16)
    total = None
    for k in range(2):
        hot = (slots == places[k : k + 1, :]).astype(F32).astype(BF16)
        picked = lax.dot_general(
            both, hot, (((0,), (0,)), ((), ())), preferred_element_type=F32
        )
        picked = picked * weights[k : k + 1, :]
        total = picked if total is None else total + picked
    partial[...] = total.astype(BF16)


def local(tokens, pre_gain, expert_gate, expert_up, expert_down, routes, route_weights, post_gain):
    groups = lax.axis_size("ep")
    columns = lax.axis_size("z8")
    tok_rows, part_width = tokens.shape
    full_width = part_width * lax.axis_size(TP)
    width = full_width // 4
    few = 3 * tok_rows // groups // 2
    slots_all = 2 * groups * few
    units = expert_gate.shape[-1]

    lanes = tok_rows // 2
    copies, places, dispatch = kernel(
        spread_kernel,
        [
            jax.ShapeDtypeStruct((columns, 2 * part_width + 8, lanes), BF16),
            jax.ShapeDtypeStruct((2, tok_rows), jnp.int32),
            jax.ShapeDtypeStruct((slots_all, tok_rows), BF16),
        ],
        in_hbm(tokens.T),
        in_hbm(pre_gain[None]),
        in_hbm(routes.T),
        in_specs=[HBM] * 3,
        scratch_shapes=[
            pltpu.VMEM((part_width, tok_rows), BF16),
            pltpu.VMEM((1, part_width), F32),
            pltpu.VMEM((2, tok_rows), jnp.int32),
            pltpu.VMEM((2 * part_width + 8, lanes), BF16),
            pltpu.SemaphoreType.DMA((3,)),
        ],
    )
    gathered = exchanged(copies, "z8")

    outgoing = kernel(
        dispatch_kernel,
        pltpu.HBM((2, slots_all, width), BF16),
        dispatch,
        gathered,
        out_specs=HBM,
        scratch_shapes=[pltpu.VMEM((slots_all, width), BF16), pltpu.SemaphoreType.DMA((2, 4))],
    )
    rows = exchanged(outgoing.reshape(4 * groups, few, width), ("zp", "core", "ep"))

    gain = gathered[:, 2 * part_width : 2 * part_width + 3, :part_width].astype(F32)
    gain = gain.sum(axis=1).reshape(1, width)
    gain = lax.all_gather(gain, ("zp", "core"), axis=0, tiled=True)

    gate = expert_gate.reshape(columns, 4, part_width, units)
    up = expert_up.reshape(columns, 4, part_width, units)
    down, gate_head = kernel(
        reorder_kernel,
        [
            pltpu.HBM((4, units, width), BF16),
            jax.ShapeDtypeStruct((5, *gate.shape[1:]), BF16),
        ],
        in_hbm(expert_down.reshape(units, full_width)),
        in_hbm(gate),
        in_specs=[HBM] * 2,
        out_specs=[HBM, VMEM],
        scratch_shapes=[
            pltpu.VMEM((units, full_width), BF16),
            pltpu.VMEM((4, units, width), BF16),
            pltpu.SemaphoreType.DMA((3,)),
        ],
    )
    gate_peer = swapped(gate)
    up_peer = swapped(up)
    down_peer = swapped(down)
    sent = kernel(
        expert_kernel,
        jax.ShapeDtypeStruct((4, groups * few, width), BF16),
        rows.reshape(4, groups * few, width),
        gain,
        gate_head,
        in_hbm(gate),
        in_hbm(up),
        gate_peer,
        in_hbm(up_peer),
        in_hbm(down),
        in_hbm(down_peer),
        in_specs=[VMEM] * 3 + [HBM] * 2 + [VMEM] + [HBM] * 3,
        scratch_shapes=[pltpu.VMEM(gate.shape, BF16)] * 3
        + [pltpu.VMEM(down.shape, BF16)] * 2
        + [pltpu.VMEM((groups * few, full_width), BF16), pltpu.SemaphoreType.DMA((5,))],
    )
    returned = exchanged(sent.reshape(4 * groups, few, width), ("zp", "core", "ep"))

    partial = kernel(
        combine_kernel,
        jax.ShapeDtypeStruct((width, tok_rows), BF16),
        returned.reshape(2, slots_all, width),
        places,
        route_weights.T,
    )
    parts = exchanged(partial.reshape(columns, part_width, tok_rows), "z8")
    combined = jnp.sum(parts.astype(F32), axis=0)
    own_sq = jnp.sum(combined * combined, axis=0)
    copies = jnp.broadcast_to(own_sq[None, None], (lax.axis_size(TP), 1, tok_rows))
    output_sq = jnp.sum(exchanged(copies, TP), axis=(0, 1))
    result = combined * lax.rsqrt(output_sq / full_width + EPSILON) * post_gain[:, None]
    return result.astype(BF16).T


def solution(mesh):
    torus = Mesh(mesh.devices.reshape(mesh.shape["ep"], 8, 2, 2), ("ep", *TP))
    in_specs = (
        P("ep", TP),
        P(TP),
        P("ep", None, TP),
        P("ep", None, TP),
        P("ep", TP, None),
        P("ep", None),
        P("ep", None),
        P(TP),
    )

    return jax.shard_map(
        local, mesh=torus, in_specs=in_specs, out_specs=P("ep", TP), check_vma=False
    )
```
